32 devices in a mesh: grp: 2 (over x), ep: 8 (over z, y), tp: 2 (over core).
Axes of the slice: x: 2, y: 2, z: 4, core: 2. Of those that a mesh axis runs over, the one named last changes fastest.
Arguments:
- tokens: bfloat16 [8192, 2048], P(('grp', 'ep', 'tp')), parts along dimension 0, may hold values from -6 to 6
- norm_gain: float32 [2048], replicated, may hold values from 0.1 to 1.9
- expert_ids: int32 [8192, 4], P(('grp', 'ep', 'tp')), parts along dimension 0, may hold values from 0 to 31, all different within a row; in each aligned block of 256 rows (0 to 255, 256 to 511, ...) at most 40 rows name the same one
- gate_weights: float32 [8192, 4], P(('grp', 'ep', 'tp')), parts along dimension 0, may hold values from 0.1 to 1
- expert_gate: bfloat16 [32, 2048, 512], P('ep', None, 'tp'), may hold values from -0.125 to 0.125
- expert_up: bfloat16 [32, 2048, 512], P('ep', None, 'tp'), may hold values from -0.125 to 0.125
- expert_down: bfloat16 [32, 512, 2048], P('ep', 'tp'), may hold values from -0.25 to 0.25
- shared_gate: bfloat16 [2048, 512], replicated, may hold values from -0.125 to 0.125
- shared_up: bfloat16 [2048, 512], replicated, may hold values from -0.125 to 0.125
- shared_down: bfloat16 [512, 2048], replicated, may hold values from -0.25 to 0.25
- post_gain: float32 [2048], replicated, may hold values from 0.1 to 1.9
Outputs:
- mixed: bfloat16 [8192, 2048], P(('grp', 'ep', 'tp')), parts along dimension 0
The draws below stay inside these ranges and needn't reach their ends.
There are 2 independent parts, one for each index of `grp`. The reference program is written for one: setup_inputs(seed, part) draws one part's arguments, and reference() takes and returns one part's arrays. A program takes and returns all parts, laid end to end along the dimension named above; an argument that names none is the same for every part. Nothing has to cross between parts.
Inputs may be any that keep to these rules, and one draw needn't show every extreme that they name: `expert_ids`: each row names 4 different experts; in each device's aligned block of 256 rows no expert is named by more than 40 rows, a bound that some block reaches.
All inputs are finite; a program needn't handle non-finite values.
Results may differ from the reference program's by a relative error of at most 0.0067.
Values may be sent and summed in bfloat16 or wider, within the bound.
No kernel may reach another device: no remote copies, remote signals or barrier semaphores. Data moves between devices by JAX's collectives and lax.ppermute only.
A program may use at most 128 MiB of HBM per device.

```python
import math
import jax
import jax.numpy as jnp
import numpy as np
from jax import lax

D = 2048
FE = 512
FS = 512
EXPERTS = 32
TOP_K = 4
TOK_DEV = 256
CAP = 40
TOKENS = 4096


def shard_levels(stream_key, dims, split, low, top_value):
    def one(axis_at, blocks):
        heights = jax.random.uniform(jax.random.fold_in(jax.random.fold_in(stream_key, 6), axis_at), (blocks,), jnp.float32, low / len(split), top_value / len(split))
        return jnp.repeat(jnp.exp(heights), dims[axis_at] // blocks).reshape((-1,) + (1,) * (len(dims) - axis_at - 1))

    level = one(*split[0])
    for cut in split[1:]:
        level = level * one(*cut)
    return level


def assign_block(rng, own, number, rows, amount, top, limit, lean):
    sequence = jax.random.permutation(rng, amount)
    heavy_load, common = load_shares(amount, rows * top, limit, lean, True), load_shares(amount, rows * top, limit, lean, False)
    places = jnp.arange(amount)

    def named(sizes, offset_by):
        used = int((sizes > 0).sum())
        fixed = max(1, used // 4)
        moved = fixed + (places - fixed + offset_by * (used - fixed)) % max(1, amount - fixed)
        return jnp.zeros((amount,), jnp.int32).at[sequence[jnp.where(places < fixed, places, moved)]].set(jnp.asarray(sizes, jnp.int32))

    sizes = jnp.where(number % 4 == 0, named(heavy_load, number // 4), named(common, number - number // 4 - 1))
    mixed = jax.random.permutation(jax.random.fold_in(own, 3), amount)
    source_of, taker = mixed[0:amount // 2 * 2:2], mixed[1:amount // 2 * 2:2]
    margin = jnp.minimum(sizes[source_of] - 1, limit - sizes[taker]) // 2
    margin = jnp.where((source_of == sequence[0]) | (taker == sequence[0]) | (sizes[taker] == 0), 0, jnp.maximum(margin, 0))
    moved = jax.random.randint(jax.random.fold_in(own, 4), (amount // 2,), 0, 1 << 20) % (margin + 1)
    sizes = sizes.at[source_of].add(-moved).at[taker].add(moved)
    items = jnp.searchsorted(jnp.cumsum(sizes), jnp.arange(rows * top), side="right").astype(jnp.int32)
    table = items.reshape(top, rows).T
    table = table[jax.random.permutation(jax.random.fold_in(own, 1), rows)]
    offset_by = jax.random.randint(jax.random.fold_in(own, 2), (rows, 1), 0, top)
    return jnp.take_along_axis(table, (jnp.arange(top)[None, :] + offset_by) % top, axis=1)


def load_shares(number_of, total, bound, skew, full):
    weights = [(1 << 20) // math.isqrt(rank ** skew) + 1 for rank in range(1, number_of + 1)]
    largest = bound if full else min(bound, max(-(-total // number_of), total * weights[0] // sum(weights)))
    least = 1 if total - largest >= number_of - 1 else 0
    holding, rest = [largest] + [least] * (number_of - 1), total - largest - least * (number_of - 1)
    while rest > 0:
        free = [i for i in range(1, number_of) if holding[i] < largest] or [i for i in range(1, number_of) if holding[i] < bound]
        pool, left = sum([weights[i] for i in free]), rest
        for i in free:
            more = min(bound - holding[i], max(1, left * weights[i] // pool), rest)
            holding[i] = holding[i] + more
            rest = rest - more
    return np.array(holding)


def gaussian(own_key, dims, scale, reach, shards=(), kind=jnp.bfloat16):
    drawn = jax.random.normal(own_key, dims, jnp.float32) * scale
    if len(shards) > 0:
        drawn = shard_levels(own_key, dims, shards, -0.22, 0.18) * drawn
    return jnp.clip(drawn, min=-reach, max=reach).astype(kind)


def setup_inputs(seed: int = 0, part: int = 0) -> dict:
    streams_of = jax.random.split(jax.random.key(seed), 12)
    own_keys = jax.random.split(jax.random.fold_in(streams_of[11], part), 12)
    tokens = gaussian(own_keys[0], (TOKENS, D), 1.0, 6.0, ((0, 16),))
    norm_gain = jnp.clip(1.0 + 0.18 * jax.random.normal(streams_of[1], (D,), jnp.float32), 0.1, 1.9)
    expert_ids_keys = jax.random.split(jax.random.fold_in(own_keys[2], 1), TOKENS // TOK_DEV)
    expert_ids_turns = jax.random.permutation(jax.random.fold_in(own_keys[2], 3), TOKENS // TOK_DEV)
    expert_ids = jax.vmap(lambda own, number: assign_block(jax.random.fold_in(own_keys[2], 2), own, number, TOK_DEV, EXPERTS, TOP_K, CAP, 1))(expert_ids_keys, expert_ids_turns).reshape((TOKENS, TOP_K))
    gate_weights = jnp.clip(jnp.exp(math.log(1.0) - 2.3025851 * jax.random.uniform(own_keys[3], (TOKENS, TOP_K), jnp.float32) ** shard_levels(own_keys[3], (TOKENS, TOP_K), ((0, 16),), -0.2, 0.2)), 0.1, 1.0)
    expert_gate = gaussian(streams_of[4], (EXPERTS, D, FE), D ** -0.5, 0.125, ((0, 8), (2, 2)))
    expert_up = gaussian(streams_of[5], (EXPERTS, D, FE), D ** -0.5, 0.125, ((0, 8), (2, 2)))
    expert_down = gaussian(streams_of[6], (EXPERTS, FE, D), FE ** -0.5, 0.25, ((0, 8), (1, 2)))
    shared_gate = gaussian(streams_of[7], (D, FS), D ** -0.5, 0.125)
    shared_up = gaussian(streams_of[8], (D, FS), D ** -0.5, 0.125)
    shared_down = gaussian(streams_of[9], (FS, D), FS ** -0.5, 0.25)
    post_gain = jnp.clip(1.0 + 0.18 * jax.random.normal(streams_of[10], (D,), jnp.float32), 0.1, 1.9)
    return dict(tokens=tokens, norm_gain=norm_gain, expert_ids=expert_ids, gate_weights=gate_weights, expert_gate=expert_gate, expert_up=expert_up, expert_down=expert_down, shared_gate=shared_gate, shared_up=shared_up, shared_down=shared_down, post_gain=post_gain)


EPS = 1e-06

def rms_scale(inputs, gain):
    mean_sq = lax.optimization_barrier(jnp.mean(inputs * inputs, axis=-1, keepdims=True))
    return inputs * lax.rsqrt(mean_sq + EPS) * gain.astype(jnp.float32)

def swiglu_out(tok_rows, w_gate, w_up, w_down):
    gate_act = jnp.dot(tok_rows, w_gate, preferred_element_type=jnp.float32)
    up_act = jnp.dot(tok_rows, w_up, preferred_element_type=jnp.float32)
    hidden = (jax.nn.silu(gate_act) * up_act).astype(jnp.bfloat16)
    return jnp.dot(hidden, w_down, preferred_element_type=jnp.float32)

def reference(tokens, norm_gain, expert_ids, gate_weights, expert_gate, expert_up, expert_down, shared_gate, shared_up, shared_down, post_gain):
    tok_total = tokens.shape[0]
    width = tokens.shape[1]
    blocks = tok_total // TOK_DEV
    normed = rms_scale(tokens.astype(jnp.float32), norm_gain).astype(jnp.bfloat16)
    ids_blocked = expert_ids.reshape(blocks, TOK_DEV * TOP_K)
    onehot = (ids_blocked[:, :, None] == jnp.arange(EXPERTS, dtype=jnp.int32)[None, None, :]).astype(jnp.int32)
    slot_index = lax.optimization_barrier(jnp.sum(jnp.cumsum(onehot, axis=1) * onehot, axis=2)) - 1
    block_index = jnp.arange(blocks, dtype=jnp.int32)[:, None]
    position = (ids_blocked * (blocks * CAP) + block_index * CAP + slot_index).reshape(-1)
    source_row = (block_index * TOK_DEV + jnp.arange(TOK_DEV * TOP_K, dtype=jnp.int32)[None, :] // TOP_K).reshape(-1)
    lookup = jnp.full((EXPERTS * blocks * CAP,), tok_total, jnp.int32).at[position].set(source_row)
    lookup = lookup.reshape(EXPERTS, blocks * CAP)
    weight_table = jnp.zeros((EXPERTS * blocks * CAP,), jnp.float32).at[position].set(gate_weights.reshape(-1))
    weight_table = weight_table.reshape(EXPERTS, blocks * CAP)
    padded = jnp.concatenate([normed, jnp.zeros((1, width), jnp.bfloat16)], axis=0)

    def add_expert(combined, inputs):
        table_rows, table_weights, w_gate, w_up, w_down = inputs
        result = swiglu_out(padded[table_rows], w_gate, w_up, w_down).astype(jnp.bfloat16)
        combined = combined.at[table_rows].add(table_weights[:, None] * result.astype(jnp.float32))
        return (combined, None)
    start = jnp.zeros((tok_total + 1, width), jnp.float32)
    combined, _ = lax.scan(add_expert, start, (lookup, weight_table, expert_gate, expert_up, expert_down))
    shared_out = swiglu_out(normed, shared_gate, shared_up, shared_down)
    combined = combined[:tok_total] + shared_out
    return rms_scale(combined, post_gain).astype(jnp.bfloat16)
```

```python
import functools

import jax
import jax.numpy as jnp
from jax import lax
from jax.experimental import pallas as pl
from jax.experimental.pallas import tpu as pltpu
from jax.sharding import PartitionSpec as P

EXPERTS = 32
CAP = 40
EPS = 1e-06
PAIR = 2
ROWS = 16


F32 = jnp.float32
BF16 = jnp.bfloat16


def dot(a, b):
    return jnp.dot(a, b, preferred_element_type=F32)


def rms_scale(inputs, gain):
    mean_sq = jnp.mean(inputs * inputs, axis=-1, keepdims=True)
    return inputs * lax.rsqrt(mean_sq + EPS) * gain


def norm_kernel(tok_ref, gain_ref, ids_ref, w_ref, out_ref):
    tok = tok_ref.shape[0]
    top = ids_ref.shape[0]
    out_ref[:tok, :] = rms_scale(tok_ref[...].astype(F32), gain_ref[...]).astype(BF16)
    experts = lax.broadcasted_iota(jnp.int32, (EXPERTS, tok), 0)
    weight = jnp.zeros((EXPERTS, tok), F32)
    named = jnp.zeros((EXPERTS, tok), F32)
    for k in range(top):
        hit = ids_ref[k : k + 1, :] == experts
        named = named + jnp.where(hit, 1.0, 0.0)
        weight = weight + jnp.where(hit, w_ref[k : k + 1, :], 0.0)
    before = lax.broadcasted_iota(jnp.int32, (tok, tok), 0) < lax.broadcasted_iota(jnp.int32, (tok, tok), 1)
    slot = dot(named.astype(BF16), jnp.where(before, 1.0, 0.0).astype(BF16))
    slot = jnp.where(named > 0.5, slot, -1.0)
    high = weight.astype(BF16)
    low = (weight - high.astype(F32)).astype(BF16)
    out_ref[tok:, :] = jnp.zeros((ROWS, out_ref.shape[1]), BF16)
    col = 0
    for table in (slot.astype(BF16), high, low):
        for row in range(0, EXPERTS, ROWS):
            out_ref[tok:, col : col + tok] = table[row : row + ROWS, :]
            col += tok


def norm_block(tokens, gain, ids_t, w_t):
    tok, width = tokens.shape
    return pl.pallas_call(
        norm_kernel,
        out_shape=jax.ShapeDtypeStruct((tok + ROWS, width), BF16),
        name="norm_block",
    )(tokens, gain.reshape(1, width), ids_t, w_t)


def slot_rows(meta_of, mine, local):
    half = local * CAP
    row = lax.broadcasted_iota(jnp.int32, (2 * half, 1), 0)
    expert = jnp.zeros_like(row)
    for i in range(1, 2 * local):
        expert = expert + jnp.where(row >= i * CAP, 1, 0)
    slot = row - expert * CAP
    other = mine + 1 - 2 * lax.rem(mine, 2)
    number = jnp.where(row < half, mine * local + expert, other * local + expert - local)
    pick = jnp.where(lax.broadcasted_iota(jnp.int32, (1, EXPERTS), 1) == number, 1.0, 0.0).astype(BF16)

    def table(index):
        total = None
        for i, at in enumerate(range(0, EXPERTS, ROWS)):
            part = dot(pick[:, at : at + ROWS], meta_of(index * (EXPERTS // ROWS) + i))
            total = part if total is None else total + part
        return total

    return table, slot.astype(F32)


def gather_kernel(count, mine_ref, *refs):
    metas, toks = refs[:count], refs[count : 2 * count]
    own_ref, out_ref, sel_ref = refs[2 * count :]
    tok = toks[0].shape[0]
    local, cap, _ = own_ref.shape

    @pl.when(pl.program_id(0) == 0)
    def _():
        def meta_of(group):
            cols = slice(group * tok, (group + 1) * tok)
            block = metas[0][:, cols]
            for m in metas[1:]:
                block = block + m[:, cols]
            return block

        table, slot = slot_rows(meta_of, mine_ref[0], local)
        sel_ref[...] = jnp.where(table(0) == slot, 1.0, 0.0).astype(BF16)

    block = toks[0][...]
    for t in toks[1:]:
        block = block + t[...]
    rows = dot(sel_ref[...], block)
    half = local * cap
    for e in range(local):
        own_ref[e] = rows[e * cap : (e + 1) * cap].astype(BF16)
        out_ref[e] = rows[half + e * cap : half + (e + 1) * cap].astype(BF16)


def gather(mine, blocks, local, step):
    tok, width = blocks[0].shape[0] - ROWS, blocks[0].shape[1]
    piece = pl.BlockSpec((local, CAP, step), lambda j: (0, 0, j))
    count = len(blocks)
    return pl.pallas_call(
        functools.partial(gather_kernel, count),
        grid=(width // step,),
        in_specs=[pl.BlockSpec(memory_space=pltpu.SMEM)]
        + [pl.BlockSpec((ROWS, width), lambda j: (tok // ROWS, 0))] * count
        + [pl.BlockSpec((tok, step), lambda j: (0, j))] * count,
        out_specs=[piece, piece],
        out_shape=[jax.ShapeDtypeStruct((local, CAP, width), BF16)] * 2,
        scratch_shapes=[pltpu.VMEM((2 * local * CAP, tok), BF16)],
        cost_estimate=pl.CostEstimate(flops=4 * local * CAP * tok * width, bytes_accessed=5 * tok * width, transcendentals=0),
        name="gather_rows",
    )(mine, *blocks, *blocks)


def expert_kernel(count, *refs):
    xs = refs[:count]
    gate_a, gate_b, up_a, up_b, down_a, down_b = refs[count : count + 6]
    ys = refs[count + 6 :]
    cap = xs[0].shape[1]
    rows = jnp.concatenate([x[0].astype(F32) for x in xs], axis=0).astype(BF16)
    total = None
    for gate, up, down in ((gate_a, up_a, down_a), (gate_b, up_b, down_b)):
        act = dot(rows, gate[0])
        lift = dot(rows, up[0])
        hidden = (act / (1.0 + jnp.exp(-act)) * lift).astype(BF16)
        part = dot(hidden, down[0])
        total = part if total is None else total + part
    for i, y in enumerate(ys):
        y[0] = total[i * cap : (i + 1) * cap].astype(BF16)


def experts(xs, weights):
    local, cap, width = xs[0].shape
    half = weights[0].shape[2]
    count = len(xs)
    row_spec = pl.BlockSpec((1, cap, width), lambda e: (e, 0, 0))
    in_spec = pl.BlockSpec((1, width, half), lambda e: (e, 0, 0))
    down_spec = pl.BlockSpec((1, half, width), lambda e: (e, 0, 0))
    return pl.pallas_call(
        functools.partial(expert_kernel, count),
        grid=(local,),
        in_specs=[row_spec] * count + [in_spec] * 4 + [down_spec] * 2,
        out_specs=[row_spec] * count,
        out_shape=[jax.ShapeDtypeStruct((local, cap, width), BF16)] * count,
        cost_estimate=pl.CostEstimate(
            flops=12 * count * local * cap * width * half, bytes_accessed=12 * local * width * half, transcendentals=0
        ),
        name="expert_rows",
    )(*xs, *weights)


def combine_kernel(with_base, mine_ref, count, *refs):
    metas = refs[:count]
    own_ref, back_ref = refs[count : count + 2]
    rest = refs[count + 2 :]
    base_ref = rest[0] if with_base else None
    out_ref, high_ref, low_ref = rest[-3:]
    tok = out_ref.shape[0]
    local, cap, _ = own_ref.shape

    @pl.when(pl.program_id(0) == 0)
    def _():
        def meta_of(group):
            cols = slice(group * tok, (group + 1) * tok)
            block = metas[0][:, cols]
            for m in metas[1:]:
                block = block + m[:, cols]
            return block

        table, slot = slot_rows(meta_of, mine_ref[0], local)
        here = table(0) == slot
        high_ref[...] = jnp.where(here, table(1), 0.0).T.astype(BF16)
        low_ref[...] = jnp.where(here, table(2), 0.0).T.astype(BF16)

    rows = jnp.concatenate([r[e].astype(F32) for r in (own_ref, back_ref) for e in range(local)], axis=0).astype(BF16)
    total = dot(high_ref[...], rows) + dot(low_ref[...], rows)
    if with_base:
        total = total + base_ref[...]
    out_ref[...] = total.astype(out_ref.dtype)


def combine(mine, blocks, own, back, step, base=None):
    tok, width = blocks[0].shape[0] - ROWS, blocks[0].shape[1]
    local = own.shape[0]
    count = len(blocks)
    piece = pl.BlockSpec((local, CAP, step), lambda j: (0, 0, j))
    column = pl.BlockSpec((tok, step), lambda j: (0, j))
    bases = () if base is None else (base,)

    def kernel(mine_ref, *refs):
        combine_kernel(base is not None, mine_ref, count, *refs)

    return pl.pallas_call(
        kernel,
        grid=(width // step,),
        in_specs=[pl.BlockSpec(memory_space=pltpu.SMEM)]
        + [pl.BlockSpec((ROWS, width), lambda j: (tok // ROWS, 0))] * count
        + [piece, piece]
        + [column] * len(bases),
        out_specs=column,
        out_shape=jax.ShapeDtypeStruct((tok, width), BF16 if base is None else F32),
        scratch_shapes=[pltpu.VMEM((tok, 2 * local * CAP), BF16)] * 2,
        cost_estimate=pl.CostEstimate(flops=8 * local * CAP * tok * width, bytes_accessed=5 * tok * width, transcendentals=0),
        name="combine_rows",
    )(mine, *blocks, own, back, *bases)


def shared_kernel(x_ref, gate_ref, up_ref, down_ref, out_ref):
    act = dot(x_ref[...], gate_ref[...])
    lift = dot(x_ref[...], up_ref[...])
    hidden = (act / (1.0 + jnp.exp(-act)) * lift).astype(BF16)
    part = dot(hidden, down_ref[...])

    @pl.when(pl.program_id(0) == 0)
    def _():
        out_ref[...] = part

    @pl.when(pl.program_id(0) > 0)
    def _():
        out_ref[...] += part


def shared_block(block, gate, up, down, parts):
    tok, width = block.shape[0] - ROWS, block.shape[1]
    hidden = gate.shape[1]
    step = hidden // parts
    return pl.pallas_call(
        shared_kernel,
        grid=(parts,),
        in_specs=[
            pl.BlockSpec((tok, width), lambda h: (0, 0)),
            pl.BlockSpec((width, step), lambda h: (0, h)),
            pl.BlockSpec((width, step), lambda h: (0, h)),
            pl.BlockSpec((step, width), lambda h: (h, 0)),
        ],
        out_specs=pl.BlockSpec((tok, width), lambda h: (0, 0)),
        out_shape=jax.ShapeDtypeStruct((tok, width), F32),
        cost_estimate=pl.CostEstimate(flops=6 * tok * width * hidden, bytes_accessed=6 * width * hidden, transcendentals=0),
        name="shared_expert",
    )(block, gate, up, down)


def finish_kernel(base_ref, gain_ref, *refs):
    total = base_ref[...]
    for part in refs[:-1]:
        total = total + part[...].astype(F32)
    refs[-1][...] = rms_scale(total, gain_ref[...]).astype(BF16)


def finish(base, gain, parts, step):
    tok, width = base.shape
    rows = pl.BlockSpec((step, width), lambda i: (i, 0))
    return pl.pallas_call(
        finish_kernel,
        grid=(tok // step,),
        in_specs=[rows, pl.BlockSpec((1, width), lambda i: (0, 0))] + [rows] * len(parts),
        out_specs=rows,
        out_shape=jax.ShapeDtypeStruct((tok, width), BF16),
        name="finish",
    )(base, gain.reshape(1, width), *parts)


def line_body(
    line,
    tokens,
    norm_gain,
    expert_ids,
    gate_weights,
    expert_gate,
    expert_up,
    expert_down,
    shared_gate,
    shared_up,
    shared_down,
    post_gain,
):
    local = expert_gate.shape[0]
    mine = lax.axis_index("ep").astype(jnp.int32).reshape(1)
    chip = lambda z, y: z * PAIR + y
    send = lambda x, pairs: lax.ppermute(x, "ep", pairs)
    along = lambda moves: [(chip(a, y), chip(b, y)) for a, b in moves for y in range(PAIR)]
    across = lambda places: [(chip(z, y), chip(z, 1 - y)) for z in places for y in range(PAIR)]
    swap = lambda x: lax.ppermute(x, "tp", [(0, 1), (1, 0)])

    block = norm_block(tokens, norm_gain, expert_ids.T, gate_weights.T)

    slots = []
    ups = downs = near = (block,)
    for d in range(1, line):
        up_moves = [(z, z + 1) for z in range(d - 1, line - 1)]
        down_moves = [(z, z - 1) for z in range(1, line - d + 1)]
        up_home = [(z, z - d) for z in range(d, line)]
        down_home = [(z, z + d) for z in range(line - d)]
        if 2 * d < line:
            ups = (send(ups[0], along(up_moves)),)
            downs = (send(downs[0], along(down_moves)),)
            slots.append((ups, up_home))
            slots.append((downs, down_home))
            near = near if d > 1 else ups + downs
        else:
            moves = up_home + down_home
            if d == line - 1:
                far, _ = lax.optimization_barrier((block, near))
                slots.append(((send(far, along([(b, a) for a, b in moves])),), moves))
            else:
                ups = (send(ups[0], along(up_moves)),)
                downs = (send(downs[0], along(down_moves)),)
                slots.append((ups + downs, moves))

    whole = [w for x in (expert_gate, expert_up, expert_down) for w in (x, swap(x))]
    step = tokens.shape[1] // 4

    def run(arrays_of, places_of):
        pairs = [gather(mine, a, local, step) for a in arrays_of]
        theirs = [send(p[1], across(places)) for p, places in zip(pairs, places_of)]
        xs = [x for p, t in zip(pairs, theirs) for x in (p[0], t)]
        ys = experts(xs, whole)
        backs = [send(ys[2 * i + 1], across(places)) for i, places in enumerate(places_of)]
        return [(ys[2 * i], backs[i]) for i in range(len(pairs))]

    shared = shared_block(block, shared_gate, shared_up, shared_down, 2)
    ((own, back),) = run([(block,)], [range(line)])
    base = combine(mine, (block,), own, back, step, shared)

    parts = []
    for arrays, home in slots:
        places = sorted({a for a, _ in home})
        ((own, back),) = run([arrays], [places])
        parts.append(send(combine(mine, arrays, own, back, step), along(home)))
    return finish(base, post_gain, parts, tokens.shape[0] // 4)


def expert_rows(tok_rows, w_gate, w_up, w_down):
    gate_act = jnp.einsum("erd,edf->erf", tok_rows, w_gate, preferred_element_type=jnp.float32)
    up_act = jnp.einsum("erd,edf->erf", tok_rows, w_up, preferred_element_type=jnp.float32)
    hidden = (jax.nn.silu(gate_act) * up_act).astype(jnp.bfloat16)
    return jnp.einsum("erf,efd->erd", hidden, w_down, preferred_element_type=jnp.float32)


def shared_branch(normed, shared_gate, shared_up, shared_down):
    shared_act = jnp.dot(normed, shared_gate, preferred_element_type=jnp.float32)
    shared_lift = jnp.dot(normed, shared_up, preferred_element_type=jnp.float32)
    shared_hidden = (jax.nn.silu(shared_act) * shared_lift).astype(jnp.bfloat16)
    return jnp.dot(shared_hidden, shared_down, preferred_element_type=jnp.float32)


def exchange_body(
    tokens,
    norm_gain,
    expert_ids,
    gate_weights,
    expert_gate,
    expert_up,
    expert_down,
    shared_gate,
    shared_up,
    shared_down,
    post_gain,
):
    tok_count = tokens.shape[0]
    top_count = expert_ids.shape[1]
    width = tokens.shape[1]
    normed = rms_scale(tokens.astype(jnp.float32), norm_gain).astype(jnp.bfloat16)
    flat_ids = expert_ids.reshape(-1)
    onehot = (flat_ids[:, None] == jnp.arange(EXPERTS, dtype=jnp.int32)[None, :]).astype(jnp.int32)
    slot_index = jnp.sum(jnp.cumsum(onehot, axis=0) * onehot, axis=1) - 1
    position = flat_ids * CAP + slot_index
    source_row = jnp.arange(tok_count * top_count, dtype=jnp.int32) // top_count
    lookup = jnp.full((EXPERTS * CAP,), tok_count, jnp.int32).at[position].set(source_row)
    padded = jnp.concatenate([normed, jnp.zeros((1, width), jnp.bfloat16)], axis=0)
    outgoing = padded[lookup].reshape(EXPERTS, 1, CAP, width)
    whole_gate, whole_up, whole_down = (
        lax.all_gather(expert_gate, "tp", axis=2, tiled=True),
        lax.all_gather(expert_up, "tp", axis=2, tiled=True),
        lax.all_gather(expert_down, "tp", axis=1, tiled=True),
    )
    arrived = lax.all_to_all(outgoing, "ep", split_axis=0, concat_axis=1, tiled=True)
    local_experts = arrived.shape[0]
    senders = arrived.shape[1]
    slots = arrived.shape[2]
    tok_rows = arrived.reshape(local_experts, senders * slots, width)
    result = expert_rows(tok_rows, whole_gate, whole_up, whole_down).astype(jnp.bfloat16)
    result = result.reshape(local_experts, senders, slots, width)
    returned = lax.all_to_all(result, "ep", split_axis=1, concat_axis=0, tiled=True)
    shared_out = shared_branch(normed, shared_gate, shared_up, shared_down)
    back_rows = returned.reshape(EXPERTS * CAP, width)
    picked = back_rows[position].reshape(tok_count, top_count, width).astype(jnp.float32)
    routed = jnp.einsum("tk,tkd->td", gate_weights, picked)
    combined = routed + shared_out
    return rms_scale(combined, post_gain).astype(jnp.bfloat16)


def body(*args):
    tokens, expert_gate = args[0], args[4]
    ep = lax.axis_size("ep")
    if ep % PAIR == 0 and expert_gate.shape[0] * CAP * PAIR >= tokens.shape[0]:
        return line_body(ep // PAIR, *args)
    return exchange_body(*args)


def solution(mesh):
    return jax.shard_map(
        body,
        mesh=mesh,
        in_specs=(
            P(("grp", "ep", "tp"), None),
            P(),
            P(("grp", "ep", "tp"), None),
            P(("grp", "ep", "tp"), None),
            P("ep", None, "tp"),
            P("ep", None, "tp"),
            P("ep", "tp", None),
            P(),
            P(),
            P(),
            P(),
        ),
        out_specs=P(("grp", "ep", "tp"), None),
        check_vma=False,
    )
```
